32 devices in a mesh: ep: 8 (over z, y), tp: 4 (over x, core).
Axes of the slice: x: 2, y: 2, z: 4, core: 2. Of those that a mesh axis runs over, the one named last changes fastest.
Arguments:
- tokens: bfloat16 [1024, 2048], P('ep'), may hold values from -36 to 36, as said below
- norm_gain: float32 [2048], replicated, may hold values from 0.1 to 1.9
- chosen: int32 [8, 256], replicated, may hold values from 0 to 1023, as said below
- slot_weight: float32 [8, 256], replicated, may hold values from 0.1 to 1
- gate_weight: bfloat16 [8, 2048, 4096], P(None, 'ep', 'tp'), may hold values from -0.125 to 0.125
- up_weight: bfloat16 [8, 2048, 4096], P(None, 'ep', 'tp'), may hold values from -0.125 to 0.125
- down_weight: bfloat16 [8, 2048, 4096], P(None, 'ep', 'tp'), may hold values from -0.09375 to 0.09375
Outputs:
- mixed: bfloat16 [1024, 2048], P('ep', 'tp')
The draws below stay inside these ranges and needn't reach their ends.
Inputs may be any that keep to these rules, and one draw needn't show every extreme that they name: `tokens`: each entry is the scaled entry of a bounded draw; rows and features differ in scale. `chosen`: the 256 slots of an expert name distinct tokens. Slots of an expert fall into aligned blocks of 256; within a block the token numbers ascend, and at most 64 of them lie among the 128 tokens of one index of ep (tokens i * 128 onward belong to index i); in every block some index supplies exactly 64.
All inputs are finite; a program needn't handle non-finite values.
Results may differ from the reference program's by a relative error of at most 0.019.
Values may be sent and summed in bfloat16 or wider, within the bound.
No kernel may reach another device: no remote copies, remote signals or barrier semaphores. Data moves between devices by JAX's collectives and lax.ppermute only.
A program may use at most 64 MiB of HBM per device.

```python
import math
import jax
import jax.numpy as jnp
from jax import lax

D = 2048
FF = 4096
EXPERTS = 8
TOK_DEV = 128
TOKENS = 1024
CAP = 256
SLOTS_DEV = 256
SLOT_CAP = 64
N_TP = 4


def draw_tokens(key, part):
    row_key, column_key, base_key = jax.random.split(jax.random.fold_in(key, 3), 3)
    row_scale = jnp.exp(jax.random.uniform(row_key, (TOKENS, 1), jnp.float32, math.log(0.3), math.log(3.0)))
    column_scale = jnp.exp(jax.random.uniform(column_key, (1, D), jnp.float32, math.log(0.3), math.log(3.0)))
    base = jax.random.normal(base_key, (TOKENS, D), jnp.float32)
    base = jnp.clip(base, -4.0, 4.0)
    return (base * row_scale * column_scale).astype(jnp.bfloat16)


def draw_chosen(key, part):
    owners_total = TOKENS // TOK_DEV
    group_size = owners_total // EXPERTS
    seats_total = owners_total * SLOT_CAP
    order_key, seat_key, forced_key = jax.random.split(jax.random.fold_in(key, 17), 3)
    order_scores = jax.random.randint(order_key, (EXPERTS, owners_total, TOK_DEV), 0, 1 << 20) * TOK_DEV
    order_scores = order_scores + jnp.arange(TOK_DEV, dtype=jnp.int32)
    token_order = jnp.argsort(order_scores, axis=-1).astype(jnp.int32)
    seat_scores = jax.random.randint(seat_key, (owners_total, seats_total), 0, 1 << 20) * seats_total
    seat_scores = seat_scores + jnp.arange(seats_total, dtype=jnp.int32)
    forced_owner = jax.random.randint(forced_key, (owners_total, 1), 0, owners_total)
    seat_owner_all = jnp.arange(seats_total, dtype=jnp.int32) // SLOT_CAP
    seat_scores = jnp.where(seat_owner_all[None, :] == forced_owner, seat_scores - (1 << 30), seat_scores)
    picked_seats = jnp.argsort(seat_scores, axis=-1)[:, :SLOTS_DEV].astype(jnp.int32)
    seat_owner = picked_seats // SLOT_CAP
    seat_rank = picked_seats % SLOT_CAP
    piece_index = jnp.arange(owners_total, dtype=jnp.int32)[:, None]
    expert_index = piece_index // group_size
    within = piece_index % group_size * SLOT_CAP + seat_rank
    local_token = token_order[expert_index, seat_owner, within]
    global_token = seat_owner * TOK_DEV + local_token
    return jnp.sort(global_token, axis=-1).reshape(EXPERTS, CAP).astype(jnp.int32)


def steps_of(rng, dims, cuts, least, largest):
    def one(position, shards_of):
        heights = jax.random.uniform(jax.random.fold_in(jax.random.fold_in(rng, 6), position), (shards_of,), jnp.float32, least / len(cuts), largest / len(cuts))
        return jnp.repeat(jnp.exp(heights), dims[position] // shards_of).reshape((-1,) + (1,) * (len(dims) - position - 1))

    factor_of = one(*cuts[0])
    for cut in cuts[1:]:
        factor_of = factor_of * one(*cut)
    return factor_of


def noise(key, dims, deviation, reach, shards=(), kind=jnp.bfloat16):
    values = jax.random.normal(key, dims, jnp.float32) * deviation
    if len(shards) > 0:
        values = steps_of(key, dims, shards, -0.22, 0.18) * values
    return jnp.clip(values, min=-reach, max=reach).astype(kind)


def setup_inputs(seed: int = 0) -> dict:
    key_of = jax.random.split(jax.random.key(seed), 8)
    return {
        "tokens": draw_tokens(jax.random.fold_in(key_of[7], 71), 0),
        "norm_gain": jnp.clip(1.0 + 0.18 * jax.random.normal(key_of[1], (D,), jnp.float32), 0.1, 1.9),
        "chosen": draw_chosen(jax.random.fold_in(key_of[7], 71), 0),
        "slot_weight": jnp.clip(jnp.exp(jax.random.uniform(key_of[3], (EXPERTS, CAP), jnp.float32, math.log(0.1), math.log(1.0))), 0.1, 1.0),
        "gate_weight": noise(key_of[4], (EXPERTS, D, FF), D ** -0.5, 0.125, ((1, 8), (2, 4))),
        "up_weight": noise(key_of[5], (EXPERTS, D, FF), D ** -0.5, 0.125, ((1, 8), (2, 4))),
        "down_weight": noise(key_of[6], (EXPERTS, D, FF), FF ** -0.5, 0.09375, ((1, 8), (2, 4))),
    }


EPSILON = 1e-06

def reference(tokens, norm_gain, chosen, slot_weight, gate_weight, up_weight, down_weight):
    values = tokens.astype(jnp.float32)
    scaled = values * lax.rsqrt(lax.optimization_barrier(jnp.mean(values * values, axis=1, keepdims=True)) + EPSILON)
    normed = (scaled * norm_gain).astype(jnp.bfloat16)
    block_units = FF // N_TP

    def per_expert(accumulated, operands):
        picked, weights, gate_w, up_w, down_w = operands
        gathered = jnp.take(normed, picked, axis=0)
        gate_part = jnp.dot(gathered, gate_w, preferred_element_type=jnp.float32)
        up_part = jnp.dot(gathered, up_w, preferred_element_type=jnp.float32)
        hidden = (jax.nn.silu(gate_part) * up_part).astype(jnp.bfloat16)

        def add_block(running, block_index):
            hidden_block = lax.dynamic_slice_in_dim(hidden, block_index * block_units, block_units, 1)
            down_block = lax.dynamic_slice_in_dim(down_w, block_index * block_units, block_units, 1)
            partial_value = jnp.dot(hidden_block, down_block.T, preferred_element_type=jnp.float32).astype(jnp.bfloat16)
            partial_value = lax.optimization_barrier(partial_value)
            return (running + partial_value.astype(jnp.float32), None)
        summed, _ = lax.scan(add_block, jnp.zeros((CAP, D), jnp.float32), jnp.arange(N_TP, dtype=jnp.int32))
        expert_out = summed.astype(jnp.bfloat16)
        contribution = weights[:, None] * expert_out.astype(jnp.float32)
        return (accumulated.at[picked].add(contribution), None)
    mixed_out, _ = lax.scan(per_expert, jnp.zeros((TOKENS, D), jnp.float32), (chosen, slot_weight, gate_weight, up_weight, down_weight))
    return mixed_out.astype(jnp.bfloat16)
```

```python
import functools

import jax
import jax.numpy as jnp
from jax import lax
from jax.experimental import pallas as pl
from jax.experimental.pallas import tpu as pltpu
from jax.sharding import PartitionSpec as P

EPSILON = 1e-06


def weights_move(tokens, norm_gain, chosen, slot_weight, gate_weight, up_weight, down_weight):
    expert_devices = lax.axis_size("ep")
    width_devices = lax.axis_size("tp")
    device_index = lax.axis_index("ep")
    width_index = lax.axis_index("tp")
    local_tokens = tokens.shape[0]
    model_width = tokens.shape[1]
    expert_total = chosen.shape[0]
    group_size = expert_devices // expert_total
    slots_piece = chosen.shape[1] // group_size
    seat_count = 4 * local_tokens // expert_devices
    buffer_rows = expert_devices * seat_count
    column_width = model_width // width_devices
    values = tokens.astype(jnp.float32)
    scaled = values * lax.rsqrt(jnp.mean(values * values, axis=1, keepdims=True) + EPSILON)
    normed = (scaled * norm_gain).astype(jnp.bfloat16)
    piece_tokens = chosen.reshape(expert_devices, slots_piece)
    piece_weights = slot_weight.reshape(expert_devices, slots_piece)
    owners = piece_tokens // local_tokens
    is_mine = owners == device_index
    earlier = jnp.sum((owners < device_index).astype(jnp.int32), axis=1, keepdims=True)
    seat_index = jnp.arange(slots_piece, dtype=jnp.int32)[None, :] - earlier
    local_index = piece_tokens - device_index * local_tokens
    seat_range = jnp.arange(seat_count, dtype=jnp.int32)
    matches = is_mine[:, None, :] & (seat_index[:, None, :] == seat_range[None, :, None])
    filled = jnp.any(matches, axis=2).reshape(buffer_rows)
    source_index = jnp.sum(jnp.where(matches, local_index[:, None, :], 0), axis=2).reshape(
        buffer_rows
    )
    seat_weight = jnp.sum(jnp.where(matches, piece_weights[:, None, :], 0.0), axis=2).reshape(
        buffer_rows
    )
    my_tokens = lax.dynamic_index_in_dim(piece_tokens, device_index, 0, keepdims=False)
    my_owners = my_tokens // local_tokens
    before = jnp.sum((my_owners[None, :] < my_owners[:, None]).astype(jnp.int32), axis=1)
    arrival_row = my_owners * seat_count + jnp.arange(slots_piece, dtype=jnp.int32) - before
    gate_send = jnp.repeat(gate_weight, group_size, axis=0)
    up_send = jnp.repeat(up_weight, group_size, axis=0)
    down_send = jnp.repeat(down_weight, group_size, axis=0)
    gate_full, up_full = (
        lax.all_to_all(gate_send, "ep", split_axis=0, concat_axis=1, tiled=True),
        lax.all_to_all(up_send, "ep", split_axis=0, concat_axis=1, tiled=True),
    )
    down_full = lax.all_to_all(down_send, "ep", split_axis=0, concat_axis=1, tiled=True)
    empty_value = jnp.zeros((), jnp.bfloat16)
    columns = lax.dynamic_slice_in_dim(normed, width_index * column_width, column_width, 1)
    outgoing = jnp.where(filled[:, None], jnp.take(columns, source_index, axis=0), empty_value)
    narrow = lax.all_to_all(
        outgoing.reshape(expert_devices, seat_count, column_width),
        "ep",
        split_axis=0,
        concat_axis=0,
        tiled=True,
    )
    arrived = lax.all_gather(narrow, "tp", axis=2, tiled=True)
    slot_rows = jnp.take(arrived.reshape(buffer_rows, model_width), arrival_row, axis=0)
    gate_part = jnp.dot(slot_rows, gate_full[0], preferred_element_type=jnp.float32)
    up_part = jnp.dot(slot_rows, up_full[0], preferred_element_type=jnp.float32)
    hidden = (jax.nn.silu(gate_part) * up_part).astype(jnp.bfloat16)
    down_rows = down_full[0]
    summed = lax.psum_scatter(
        jnp.einsum("df,bf->db", down_rows, hidden, preferred_element_type=jnp.float32).astype(
            jnp.bfloat16
        ),
        "tp",
        scatter_dimension=0,
        tiled=True,
    )
    buffer_range = jnp.arange(buffer_rows, dtype=jnp.int32)
    hits = arrival_row[None, :] == buffer_range[:, None]
    back_index = jnp.sum(
        jnp.where(hits, jnp.arange(slots_piece, dtype=jnp.int32)[None, :], 0), axis=1
    )
    expert_out = jnp.take(summed, back_index, axis=1).reshape(
        column_width, expert_devices, seat_count
    )
    returned = lax.all_to_all(expert_out, "ep", split_axis=1, concat_axis=1, tiled=True)
    token_range = jnp.arange(local_tokens, dtype=jnp.int32)
    combine = jnp.where(
        (source_index[None, :] == token_range[:, None]) & filled[None, :], seat_weight[None, :], 0.0
    )
    mixed_out = jnp.einsum(
        "tb,cb->tc",
        combine,
        returned.reshape(column_width, buffer_rows).astype(jnp.float32),
        precision=lax.Precision.HIGHEST,
    )
    return mixed_out.astype(jnp.bfloat16)


def xor_pairs(size, mask):
    return [(a, a ^ mask) for a in range(size)]


def halving_order(bits):
    order = [0]
    for s in reversed(range(bits)):
        order = [p ^ (1 << s) for p in order] + order
    return order


def gate_up_kernel(parity, tok, row0, row1, n0, n1, wg, wu, rg, ru, send, keep, own, far):
    half = send.shape[1]
    width = own.shape[1]

    @pl.when(pl.program_id(0) == 0)
    def _():
        pick0 = (tok[0] == row0[...]).astype(jnp.float32).astype(jnp.bfloat16)
        pick1 = (tok[0] == row1[...]).astype(jnp.float32).astype(jnp.bfloat16)
        rows = jnp.dot(pick0, n0[...], preferred_element_type=jnp.float32) + jnp.dot(
            pick1, n1[...], preferred_element_type=jnp.float32
        )
        even = parity[0] == 0
        low, high = rows[:, :width], rows[:, width:]
        own[...] = jnp.where(even, low, high).astype(jnp.bfloat16)
        far[...] = jnp.where(even, high, low).astype(jnp.bfloat16)

    for n, (w, r) in enumerate(((wg, rg), (wu, ru))):
        part = jnp.dot(own[...], w[0], preferred_element_type=jnp.float32) + jnp.dot(
            far[...], r[0], preferred_element_type=jnp.float32
        )
        send[n] = part[:half].astype(jnp.bfloat16)
        keep[n] = part[half:]


def gate_up(q, parity, tok, row0, row1, n0, n1, wg, wu, rg, ru):
    slots = tok.shape[1]
    width, units = wg.shape[1:]
    step = units // 2
    rows = n0.shape[0]
    whole = lambda f, s: (0, 0)
    mine = pl.BlockSpec((1, width, step), lambda f, s: (2 * q + s[0], 0, f))
    theirs = pl.BlockSpec((1, width, step), lambda f, s: (0, 0, f))
    half = slots // 2
    out = pl.BlockSpec((2, half, step), lambda f, s: (0, 0, f))
    return pl.pallas_call(
        gate_up_kernel,
        grid_spec=pltpu.PrefetchScalarGridSpec(
            num_scalar_prefetch=1,
            grid=(units // step,),
            in_specs=[
                pl.BlockSpec((1, slots, 1), lambda f, s: (q, 0, 0)),
                pl.BlockSpec((1, rows), whole),
                pl.BlockSpec((1, rows), whole),
                pl.BlockSpec(n0.shape, whole),
                pl.BlockSpec(n1.shape, whole),
                mine,
                mine,
                theirs,
                theirs,
            ],
            out_specs=[out, out],
            scratch_shapes=[pltpu.VMEM((slots, width), jnp.bfloat16)] * 2,
        ),
        out_shape=[
            jax.ShapeDtypeStruct((2, half, units), jnp.bfloat16),
            jax.ShapeDtypeStruct((2, half, units), jnp.float32),
        ],
        name=f"gate_up_{q}",
    )(parity, tok, row0, row1, n0, n1, wg, wu, rg, ru)


def down_kernel(pieces, first, last, parity, *refs):
    hid = refs[:pieces]
    tok, scale, order, wd, rd = refs[pieces : pieces + 5]
    rest = refs[pieces + 5 :]
    hidden = jnp.concatenate([h[...] for h in hid], axis=0)
    dims = (((1,), (1,)), ((), ()))
    pick = (order[...] == tok[0]).astype(jnp.float32).astype(jnp.bfloat16)
    width = wd.shape[1]
    for n, w in enumerate((wd, rd)):
        out = lax.dot_general(hidden, w[0], dims, preferred_element_type=jnp.float32)
        out = (out * scale[0]).astype(jnp.bfloat16)
        part = jnp.dot(pick, out, preferred_element_type=jnp.float32)
        cols = slice(n * width, (n + 1) * width)
        if not first:
            part = part + rest[0][:, cols]
        if last:
            half = part.shape[0] // 2
            rest[-2][:, cols] = part[:half].astype(jnp.bfloat16)
            rest[-1][:, cols] = part[half:]
        else:
            rest[-1][:, cols] = part


def down(q, last, parity, hid, tok, scale, order, wd, rd, total):
    slots = tok.shape[2]
    width, units = wd.shape[1:]
    rows = order.shape[0]
    whole = lambda g, s: (0, 0)
    in_specs = [pl.BlockSpec(h.shape, whole) for h in hid] + [
        pl.BlockSpec((1, 1, slots), lambda g, s: (q, 0, 0)),
        pl.BlockSpec((1, slots, 1), lambda g, s: (q, 0, 0)),
        pl.BlockSpec(order.shape, whole),
        pl.BlockSpec((1, width, units), lambda g, s: (2 * q + s[0], 0, 0)),
        pl.BlockSpec((1, width, units), lambda g, s: (0, 0, 0)),
    ]
    args = [parity, *hid, tok, scale, order, wd, rd]
    if total is not None:
        in_specs.append(pl.BlockSpec((rows, 2 * width), whole))
        args.append(total)
    if last:
        shape = (rows // 2, 2 * width)
        outs = [jax.ShapeDtypeStruct(shape, jnp.bfloat16), jax.ShapeDtypeStruct(shape, jnp.float32)]
    else:
        outs = [jax.ShapeDtypeStruct((rows, 2 * width), jnp.float32)]
    return pl.pallas_call(
        functools.partial(down_kernel, len(hid), total is None, last),
        grid_spec=pltpu.PrefetchScalarGridSpec(
            num_scalar_prefetch=1,
            grid=(1,),
            in_specs=in_specs,
            out_specs=[pl.BlockSpec(o.shape, whole) for o in outs],
        ),
        out_shape=outs,
        name=f"down_{q}",
    )(*args)


def sums_move(tokens, norm_gain, chosen, slot_weight, gate_weight, up_weight, down_weight):
    n_ep = lax.axis_size("ep")
    n_tp = lax.axis_size("tp")
    ep = lax.axis_index("ep")
    tp = lax.axis_index("tp")
    y, z = ep % 2, ep // 2
    core, x = tp % 2, tp // 2
    n_z = n_ep // 2
    bits = n_z.bit_length() - 1
    experts, slots = chosen.shape
    pairs = experts // 2
    tok_dev, model_width = tokens.shape
    width = gate_weight.shape[1]
    half_rows = tok_dev // 2
    columns = 2 * width
    ep_swap = lambda v, mask: lax.ppermute(v, "ep", xor_pairs(n_ep, mask))
    core_swap = lambda v: lax.ppermute(v, "tp", xor_pairs(n_tp, 1))
    parity = y.astype(jnp.int32).reshape(1)

    def swap_y(w, q):
        piece = lax.dynamic_slice_in_dim(w, 2 * q + 1 - y, 1, 0)
        return ep_swap(piece, 1)

    values = lax.dynamic_slice_in_dim(tokens, core * half_rows, half_rows, 0).astype(jnp.float32)
    scaled = values * lax.rsqrt(jnp.mean(values * values, axis=1, keepdims=True) + EPSILON)
    normed = (scaled * norm_gain).astype(jnp.bfloat16)
    parts = []
    for p in range(n_z):
        part = lax.dynamic_slice_in_dim(normed, (z ^ p) * columns, columns, 1)
        parts.append(part if p == 0 else ep_swap(part, 2 * p))
    z_rows = jnp.concatenate(parts, axis=0)
    n0 = jnp.concatenate([z_rows, ep_swap(z_rows, 1)], axis=0)
    n1 = core_swap(n0)
    r = jnp.arange(n0.shape[0], dtype=jnp.int32)
    owner = (z ^ (r // half_rows % n_z)) * 2 + (y ^ (r // (half_rows * n_z)))
    row0 = (owner * tok_dev + core * half_rows + r % half_rows)[None]
    row1 = (owner * tok_dev + (1 - core) * half_rows + r % half_rows)[None]

    order = halving_order(bits)

    def arrange(a):
        a = a.reshape(pairs, 2, n_z, slots // n_z)
        a = jnp.where(y == 0, a[:, 0], a[:, 1])
        for s in range(bits):
            b = a.reshape(pairs, n_z >> (s + 1), 2, 1 << s, slots // n_z)
            a = jnp.where((z >> s) % 2 == 0, b, jnp.flip(b, 2)).reshape(a.shape)
        return jnp.concatenate([a[:, p] for p in order], axis=1)

    tok = arrange(chosen)
    scale = arrange(slot_weight)
    tok_col, tok_row, scale_col = tok[:, :, None], tok[:, None, :], scale[:, :, None]

    yx = y * (n_tp // 2) + x
    n_far = n_ep // 2
    g = jnp.arange(n_ep * tok_dev, dtype=jnp.int32)
    side = jnp.where(g < n_far * tok_dev, 1 - core, core)
    sum_order = ((side * n_far + (yx ^ (g // tok_dev % n_far))) * tok_dev + g % tok_dev)[:, None]

    total = None
    for q in range(pairs):
        rg, ru = swap_y(gate_weight, q), swap_y(up_weight, q)
        send, keep = gate_up(
            q, parity, tok_col, row0, row1, n0, n1, gate_weight, up_weight, rg, ru
        )
        for s in range(bits):
            keep = keep + ep_swap(send, 2 << s).astype(jnp.float32)
            if s + 1 < bits:
                half = keep.shape[1] // 2
                send, keep = keep[:, :half].astype(jnp.bfloat16), keep[:, half:]
        hidden = (jax.nn.silu(keep[0]) * keep[1]).astype(jnp.bfloat16)
        hid = [hidden if p == 0 else ep_swap(hidden, 2 * p) for p in order]
        rd = swap_y(down_weight, q)
        last = q == pairs - 1
        outs = down(q, last, parity, hid, tok_row, scale_col, sum_order, down_weight, rd, total)
        total = outs[0]
    send, keep = outs
    both = keep + core_swap(send).astype(jnp.float32)
    both = both.astype(jnp.bfloat16).reshape(n_far, tok_dev, columns)
    mixed = 0.0
    for p in range(n_far):
        pairs_of = []
        for d in range(n_ep * n_tp):
            de, dt = d // n_tp, d % n_tp
            d_yx = de % 2 * (n_tp // 2) + dt // 2
            pairs_of.append((d, (dt % 2 * n_far + (d_yx ^ p)) * n_tp + de // 2))
        got = lax.ppermute(both[p], ("ep", "tp"), pairs_of).astype(jnp.float32)
        from_y = ((ep % n_far) ^ p) // (n_tp // 2)
        swapped = jnp.concatenate([got[:, width:], got[:, :width]], axis=1)
        mixed = mixed + jnp.where(from_y == 0, got, swapped)
    return mixed.astype(jnp.bfloat16)


def body(tokens, norm_gain, chosen, slot_weight, gate_weight, up_weight, down_weight):
    n_ep, n_tp = lax.axis_size("ep"), lax.axis_size("tp")
    power = n_ep >= 4 and n_ep & (n_ep - 1) == 0
    slots = chosen.shape[1]
    few = chosen.shape[0] == n_ep and slots <= 2 * gate_weight.shape[1] and slots % (4 * n_ep) == 0
    plan = sums_move if power and n_ep == 2 * n_tp and few else weights_move
    return plan(tokens, norm_gain, chosen, slot_weight, gate_weight, up_weight, down_weight)


def solution(mesh):
    in_specs = (
        P("ep", None),
        P(),
        P(),
        P(),
        P(None, "ep", "tp"),
        P(None, "ep", "tp"),
        P(None, "ep", "tp"),
    )
    out_specs = P("ep", "tp")
    return jax.shard_map(body, mesh=mesh, in_specs=in_specs, out_specs=out_specs, check_vma=False)
```

```python
import functools

import jax
import jax.numpy as jnp
from jax import lax
from jax.experimental import pallas as pl
from jax.experimental.pallas import tpu as pltpu
from jax.sharding import PartitionSpec as P

EPSILON = 1e-06


def weights_move(tokens, norm_gain, chosen, slot_weight, gate_weight, up_weight, down_weight):
    expert_devices = lax.axis_size("ep")
    width_devices = lax.axis_size("tp")
    device_index = lax.axis_index("ep")
    width_index = lax.axis_index("tp")
    local_tokens = tokens.shape[0]
    model_width = tokens.shape[1]
    expert_total = chosen.shape[0]
    group_size = expert_devices // expert_total
    slots_piece = chosen.shape[1] // group_size
    seat_count = 4 * local_tokens // expert_devices
    buffer_rows = expert_devices * seat_count
    column_width = model_width // width_devices
    values = tokens.astype(jnp.float32)
    scaled = values * lax.rsqrt(jnp.mean(values * values, axis=1, keepdims=True) + EPSILON)
    normed = (scaled * norm_gain).astype(jnp.bfloat16)
    piece_tokens = chosen.reshape(expert_devices, slots_piece)
    piece_weights = slot_weight.reshape(expert_devices, slots_piece)
    owners = piece_tokens // local_tokens
    is_mine = owners == device_index
    earlier = jnp.sum((owners < device_index).astype(jnp.int32), axis=1, keepdims=True)
    seat_index = jnp.arange(slots_piece, dtype=jnp.int32)[None, :] - earlier
    local_index = piece_tokens - device_index * local_tokens
    seat_range = jnp.arange(seat_count, dtype=jnp.int32)
    matches = is_mine[:, None, :] & (seat_index[:, None, :] == seat_range[None, :, None])
    filled = jnp.any(matches, axis=2).reshape(buffer_rows)
    source_index = jnp.sum(jnp.where(matches, local_index[:, None, :], 0), axis=2).reshape(
        buffer_rows
    )
    seat_weight = jnp.sum(jnp.where(matches, piece_weights[:, None, :], 0.0), axis=2).reshape(
        buffer_rows
    )
    my_tokens = lax.dynamic_index_in_dim(piece_tokens, device_index, 0, keepdims=False)
    my_owners = my_tokens // local_tokens
    before = jnp.sum((my_owners[None, :] < my_owners[:, None]).astype(jnp.int32), axis=1)
    arrival_row = my_owners * seat_count + jnp.arange(slots_piece, dtype=jnp.int32) - before
    gate_send = jnp.repeat(gate_weight, group_size, axis=0)
    up_send = jnp.repeat(up_weight, group_size, axis=0)
    down_send = jnp.repeat(down_weight, group_size, axis=0)
    gate_full, up_full = (
        lax.all_to_all(gate_send, "ep", split_axis=0, concat_axis=1, tiled=True),
        lax.all_to_all(up_send, "ep", split_axis=0, concat_axis=1, tiled=True),
    )
    down_full = lax.all_to_all(down_send, "ep", split_axis=0, concat_axis=1, tiled=True)
    empty_value = jnp.zeros((), jnp.bfloat16)
    columns = lax.dynamic_slice_in_dim(normed, width_index * column_width, column_width, 1)
    outgoing = jnp.where(filled[:, None], jnp.take(columns, source_index, axis=0), empty_value)
    narrow = lax.all_to_all(
        outgoing.reshape(expert_devices, seat_count, column_width),
        "ep",
        split_axis=0,
        concat_axis=0,
        tiled=True,
    )
    arrived = lax.all_gather(narrow, "tp", axis=2, tiled=True)
    slot_rows = jnp.take(arrived.reshape(buffer_rows, model_width), arrival_row, axis=0)
    gate_part = jnp.dot(slot_rows, gate_full[0], preferred_element_type=jnp.float32)
    up_part = jnp.dot(slot_rows, up_full[0], preferred_element_type=jnp.float32)
    hidden = (jax.nn.silu(gate_part) * up_part).astype(jnp.bfloat16)
    down_rows = down_full[0]
    summed = lax.psum_scatter(
        jnp.einsum("df,bf->db", down_rows, hidden, preferred_element_type=jnp.float32).astype(
            jnp.bfloat16
        ),
        "tp",
        scatter_dimension=0,
        tiled=True,
    )
    buffer_range = jnp.arange(buffer_rows, dtype=jnp.int32)
    hits = arrival_row[None, :] == buffer_range[:, None]
    back_index = jnp.sum(
        jnp.where(hits, jnp.arange(slots_piece, dtype=jnp.int32)[None, :], 0), axis=1
    )
    expert_out = jnp.take(summed, back_index, axis=1).reshape(
        column_width, expert_devices, seat_count
    )
    returned = lax.all_to_all(expert_out, "ep", split_axis=1, concat_axis=1, tiled=True)
    token_range = jnp.arange(local_tokens, dtype=jnp.int32)
    combine = jnp.where(
        (source_index[None, :] == token_range[:, None]) & filled[None, :], seat_weight[None, :], 0.0
    )
    mixed_out = jnp.einsum(
        "tb,cb->tc",
        combine,
        returned.reshape(column_width, buffer_rows).astype(jnp.float32),
        precision=lax.Precision.HIGHEST,
    )
    return mixed_out.astype(jnp.bfloat16)


def xor_pairs(size, mask):
    return [(a, a ^ mask) for a in range(size)]


def halving_order(bits):
    order = [0]
    for s in reversed(range(bits)):
        order = [p ^ (1 << s) for p in order] + order
    return order


def gate_up_kernel(parity, tok, row0, row1, n0, n1, wg, wu, rg, ru, send, keep, own, far):
    half = send.shape[1]
    width = own.shape[1]

    @pl.when(pl.program_id(0) == 0)
    def _():
        pick0 = (tok[0] == row0[...]).astype(jnp.float32).astype(jnp.bfloat16)
        pick1 = (tok[0] == row1[...]).astype(jnp.float32).astype(jnp.bfloat16)
        rows = jnp.dot(pick0, n0[...], preferred_element_type=jnp.float32) + jnp.dot(
            pick1, n1[...], preferred_element_type=jnp.float32
        )
        even = parity[0] == 0
        low, high = rows[:, :width], rows[:, width:]
        own[...] = jnp.where(even, low, high).astype(jnp.bfloat16)
        far[...] = jnp.where(even, high, low).astype(jnp.bfloat16)

    for n, (w, r) in enumerate(((wg, rg), (wu, ru))):
        part = jnp.dot(own[...], w[0], preferred_element_type=jnp.float32) + jnp.dot(
            far[...], r[0], preferred_element_type=jnp.float32
        )
        send[n] = part[:half].astype(jnp.bfloat16)
        keep[n] = part[half:]


def gate_up(q, parity, tok, row0, row1, n0, n1, wg, wu, rg, ru):
    slots = tok.shape[1]
    width, units = wg.shape[1:]
    step = units // 2
    rows = n0.shape[0]
    whole = lambda f, s: (0, 0)
    mine = pl.BlockSpec((1, width, step), lambda f, s: (2 * q + s[0], 0, f))
    theirs = pl.BlockSpec((1, width, step), lambda f, s: (0, 0, f))
    half = slots // 2
    out = pl.BlockSpec((2, half, step), lambda f, s: (0, 0, f))
    return pl.pallas_call(
        gate_up_kernel,
        grid_spec=pltpu.PrefetchScalarGridSpec(
            num_scalar_prefetch=1,
            grid=(units // step,),
            in_specs=[
                pl.BlockSpec((1, slots, 1), lambda f, s: (q, 0, 0)),
                pl.BlockSpec((1, rows), whole),
                pl.BlockSpec((1, rows), whole),
                pl.BlockSpec(n0.shape, whole),
                pl.BlockSpec(n1.shape, whole),
                mine,
                mine,
                theirs,
                theirs,
            ],
            out_specs=[out, out],
            scratch_shapes=[pltpu.VMEM((slots, width), jnp.bfloat16)] * 2,
        ),
        out_shape=[
            jax.ShapeDtypeStruct((2, half, units), jnp.bfloat16),
            jax.ShapeDtypeStruct((2, half, units), jnp.float32),
        ],
    )(parity, tok, row0, row1, n0, n1, wg, wu, rg, ru)


def down_kernel(pieces, first, last, parity, *refs):
    hid = refs[:pieces]
    tok, scale, order, wd, rd = refs[pieces : pieces + 5]
    rest = refs[pieces + 5 :]
    hidden = jnp.concatenate([h[...] for h in hid], axis=0)
    dims = (((1,), (1,)), ((), ()))
    pick = (order[...] == tok[0]).astype(jnp.float32).astype(jnp.bfloat16)
    width = wd.shape[1]
    for n, w in enumerate((wd, rd)):
        out = lax.dot_general(hidden, w[0], dims, preferred_element_type=jnp.float32)
        out = (out * scale[0]).astype(jnp.bfloat16)
        part = jnp.dot(pick, out, preferred_element_type=jnp.float32)
        cols = slice(n * width, (n + 1) * width)
        if not first:
            part = part + rest[0][:, cols]
        if last:
            half = part.shape[0] // 2
            rest[-2][:, cols] = part[:half].astype(jnp.bfloat16)
            rest[-1][:, cols] = part[half:]
        else:
            rest[-1][:, cols] = part


def down(q, last, parity, hid, tok, scale, order, wd, rd, total):
    slots = tok.shape[2]
    width, units = wd.shape[1:]
    rows = order.shape[0]
    whole = lambda g, s: (0, 0)
    in_specs = [pl.BlockSpec(h.shape, whole) for h in hid] + [
        pl.BlockSpec((1, 1, slots), lambda g, s: (q, 0, 0)),
        pl.BlockSpec((1, slots, 1), lambda g, s: (q, 0, 0)),
        pl.BlockSpec(order.shape, whole),
        pl.BlockSpec((1, width, units), lambda g, s: (2 * q + s[0], 0, 0)),
        pl.BlockSpec((1, width, units), lambda g, s: (0, 0, 0)),
    ]
    args = [parity, *hid, tok, scale, order, wd, rd]
    if total is not None:
        in_specs.append(pl.BlockSpec((rows, 2 * width), whole))
        args.append(total)
    if last:
        shape = (rows // 2, 2 * width)
        outs = [jax.ShapeDtypeStruct(shape, jnp.bfloat16), jax.ShapeDtypeStruct(shape, jnp.float32)]
    else:
        outs = [jax.ShapeDtypeStruct((rows, 2 * width), jnp.float32)]
    return pl.pallas_call(
        functools.partial(down_kernel, len(hid), total is None, last),
        grid_spec=pltpu.PrefetchScalarGridSpec(
            num_scalar_prefetch=1,
            grid=(1,),
            in_specs=in_specs,
            out_specs=[pl.BlockSpec(o.shape, whole) for o in outs],
        ),
        out_shape=outs,
    )(*args)


def sums_move(tokens, norm_gain, chosen, slot_weight, gate_weight, up_weight, down_weight):
    n_ep = lax.axis_size("ep")
    n_tp = lax.axis_size("tp")
    ep = lax.axis_index("ep")
    tp = lax.axis_index("tp")
    y, z = ep % 2, ep // 2
    core, x = tp % 2, tp // 2
    n_z = n_ep // 2
    bits = n_z.bit_length() - 1
    experts, slots = chosen.shape
    pairs = experts // 2
    tok_dev, _ = tokens.shape
    width = gate_weight.shape[1]
    half_rows = tok_dev // 2
    columns = 2 * width
    ep_swap = lambda v, mask: lax.ppermute(v, "ep", xor_pairs(n_ep, mask))
    core_swap = lambda v: lax.ppermute(v, "tp", xor_pairs(n_tp, 1))
    parity = y.astype(jnp.int32).reshape(1)

    def swap_y(w, q):
        piece = lax.dynamic_slice_in_dim(w, 2 * q + 1 - y, 1, 0)
        return ep_swap(piece, 1)

    values = lax.dynamic_slice_in_dim(tokens, core * half_rows, half_rows, 0).astype(jnp.float32)
    scaled = values * lax.rsqrt(jnp.mean(values * values, axis=1, keepdims=True) + EPSILON)
    normed = (scaled * norm_gain).astype(jnp.bfloat16)
    parts = []
    for p in range(n_z):
        part = lax.dynamic_slice_in_dim(normed, (z ^ p) * columns, columns, 1)
        parts.append(part if p == 0 else ep_swap(part, 2 * p))
    z_rows = jnp.concatenate(parts, axis=0)
    y_rows = ep_swap(z_rows, 1)
    n0 = jnp.concatenate([z_rows, y_rows], axis=0)
    n1 = core_swap(n0)
    r = jnp.arange(n0.shape[0], dtype=jnp.int32)
    owner = (z ^ (r // half_rows % n_z)) * 2 + (y ^ (r // (half_rows * n_z)))
    row0 = (owner * tok_dev + core * half_rows + r % half_rows)[None]
    row1 = (owner * tok_dev + (1 - core) * half_rows + r % half_rows)[None]

    order = halving_order(bits)

    def arrange(a):
        a = a.reshape(pairs, 2, n_z, slots // n_z)
        a = jnp.where(y == 0, a[:, 0], a[:, 1])
        for s in range(bits):
            b = a.reshape(pairs, n_z >> (s + 1), 2, 1 << s, slots // n_z)
            a = jnp.where((z >> s) % 2 == 0, b, jnp.flip(b, 2)).reshape(a.shape)
        return jnp.concatenate([a[:, p] for p in order], axis=1)

    tok = arrange(chosen)
    scale = arrange(slot_weight)
    tok_col, tok_row, scale_col = tok[:, :, None], tok[:, None, :], scale[:, :, None]

    yx = y * (n_tp // 2) + x
    n_far = n_ep // 2
    g = jnp.arange(n_ep * tok_dev, dtype=jnp.int32)
    side = jnp.where(g < n_far * tok_dev, 1 - core, core)
    sum_order = ((side * n_far + (yx ^ (g // tok_dev % n_far))) * tok_dev + g % tok_dev)[:, None]

    total = None
    for q in range(pairs):
        rg, ru = swap_y(gate_weight, q), swap_y(up_weight, q)
        send, keep = gate_up(
            q, parity, tok_col, row0, row1, n0, n1, gate_weight, up_weight, rg, ru
        )
        for s in range(bits):
            got = ep_swap(send, 2 << s)
            keep = keep + got.astype(jnp.float32)
            if s + 1 < bits:
                half = keep.shape[1] // 2
                send, keep = keep[:, :half].astype(jnp.bfloat16), keep[:, half:]
        hidden = (jax.nn.silu(keep[0]) * keep[1]).astype(jnp.bfloat16)
        hid = [hidden if p == 0 else ep_swap(hidden, 2 * p) for p in order]
        rd = swap_y(down_weight, q)
        last = q == pairs - 1
        outs = down(q, last, parity, hid, tok_row, scale_col, sum_order, down_weight, rd, total)
        total = outs[0]
    send, keep = outs
    both = keep + core_swap(send).astype(jnp.float32)
    both = both.astype(jnp.bfloat16).reshape(n_far, tok_dev, columns)
    mixed = 0.0
    for p in range(n_far):
        pairs_of = []
        for d in range(n_ep * n_tp):
            de, dt = d // n_tp, d % n_tp
            d_yx = de % 2 * (n_tp // 2) + dt // 2
            pairs_of.append((d, (dt % 2 * n_far + (d_yx ^ p)) * n_tp + de // 2))
        got = lax.ppermute(both[p], ("ep", "tp"), pairs_of).astype(jnp.float32)
        from_y = ((ep % n_far) ^ p) // (n_tp // 2)
        swapped = jnp.concatenate([got[:, width:], got[:, :width]], axis=1)
        mixed = mixed + jnp.where(from_y == 0, got, swapped)
    return mixed.astype(jnp.bfloat16)


def few_slots(n_ep, n_tp, experts, slots, width):
    power = n_ep >= 8 and n_ep & (n_ep - 1) == 0
    return (
        power
        and n_ep == 2 * n_tp
        and experts == n_ep
        and slots <= 2 * width
        and slots % (4 * n_ep) == 0
    )


def solution(mesh):
    in_specs = (
        P("ep", None),
        P(),
        P(),
        P(),
        P(None, "ep", "tp"),
        P(None, "ep", "tp"),
        P(None, "ep", "tp"),
    )
    out_specs = P("ep", "tp")
    n_ep, n_tp = mesh.shape["ep"], mesh.shape["tp"]
    mapped = functools.partial(
        jax.shard_map, mesh=mesh, in_specs=in_specs, out_specs=out_specs, check_vma=False
    )

    def step(*args):
        chosen, gate_weight = args[2], args[4]
        width = gate_weight.shape[1] // n_ep
        if not few_slots(n_ep, n_tp, *chosen.shape, width):
            return mapped(weights_move)(*args)
        return mapped(sums_move)(*args)

    return step
```

```python
import functools

import jax
import jax.numpy as jnp
from jax import lax
from jax.experimental import pallas as pl
from jax.experimental.pallas import tpu as pltpu
from jax.sharding import PartitionSpec as P

EPSILON = 1e-06


def weights_move(tokens, norm_gain, chosen, slot_weight, gate_weight, up_weight, down_weight):
    expert_devices = lax.axis_size("ep")
    width_devices = lax.axis_size("tp")
    device_index = lax.axis_index("ep")
    width_index = lax.axis_index("tp")
    local_tokens = tokens.shape[0]
    model_width = tokens.shape[1]
    expert_total = chosen.shape[0]
    group_size = expert_devices // expert_total
    slots_piece = chosen.shape[1] // group_size
    seat_count = 4 * local_tokens // expert_devices
    buffer_rows = expert_devices * seat_count
    column_width = model_width // width_devices
    values = tokens.astype(jnp.float32)
    scaled = values * lax.rsqrt(jnp.mean(values * values, axis=1, keepdims=True) + EPSILON)
    normed = (scaled * norm_gain).astype(jnp.bfloat16)
    piece_tokens = chosen.reshape(expert_devices, slots_piece)
    piece_weights = slot_weight.reshape(expert_devices, slots_piece)
    owners = piece_tokens // local_tokens
    is_mine = owners == device_index
    earlier = jnp.sum((owners < device_index).astype(jnp.int32), axis=1, keepdims=True)
    seat_index = jnp.arange(slots_piece, dtype=jnp.int32)[None, :] - earlier
    local_index = piece_tokens - device_index * local_tokens
    seat_range = jnp.arange(seat_count, dtype=jnp.int32)
    matches = is_mine[:, None, :] & (seat_index[:, None, :] == seat_range[None, :, None])
    filled = jnp.any(matches, axis=2).reshape(buffer_rows)
    source_index = jnp.sum(jnp.where(matches, local_index[:, None, :], 0), axis=2).reshape(
        buffer_rows
    )
    seat_weight = jnp.sum(jnp.where(matches, piece_weights[:, None, :], 0.0), axis=2).reshape(
        buffer_rows
    )
    my_tokens = lax.dynamic_index_in_dim(piece_tokens, device_index, 0, keepdims=False)
    my_owners = my_tokens // local_tokens
    before = jnp.sum((my_owners[None, :] < my_owners[:, None]).astype(jnp.int32), axis=1)
    arrival_row = my_owners * seat_count + jnp.arange(slots_piece, dtype=jnp.int32) - before
    gate_send = jnp.repeat(gate_weight, group_size, axis=0)
    up_send = jnp.repeat(up_weight, group_size, axis=0)
    down_send = jnp.repeat(down_weight, group_size, axis=0)
    gate_full, up_full = (
        lax.all_to_all(gate_send, "ep", split_axis=0, concat_axis=1, tiled=True),
        lax.all_to_all(up_send, "ep", split_axis=0, concat_axis=1, tiled=True),
    )
    down_full = lax.all_to_all(down_send, "ep", split_axis=0, concat_axis=1, tiled=True)
    empty_value = jnp.zeros((), jnp.bfloat16)
    columns = lax.dynamic_slice_in_dim(normed, width_index * column_width, column_width, 1)
    outgoing = jnp.where(filled[:, None], jnp.take(columns, source_index, axis=0), empty_value)
    narrow = lax.all_to_all(
        outgoing.reshape(expert_devices, seat_count, column_width),
        "ep",
        split_axis=0,
        concat_axis=0,
        tiled=True,
    )
    arrived = lax.all_gather(narrow, "tp", axis=2, tiled=True)
    slot_rows = jnp.take(arrived.reshape(buffer_rows, model_width), arrival_row, axis=0)
    gate_part = jnp.dot(slot_rows, gate_full[0], preferred_element_type=jnp.float32)
    up_part = jnp.dot(slot_rows, up_full[0], preferred_element_type=jnp.float32)
    hidden = (jax.nn.silu(gate_part) * up_part).astype(jnp.bfloat16)
    down_rows = down_full[0]
    summed = lax.psum_scatter(
        jnp.einsum("df,bf->db", down_rows, hidden, preferred_element_type=jnp.float32).astype(
            jnp.bfloat16
        ),
        "tp",
        scatter_dimension=0,
        tiled=True,
    )
    buffer_range = jnp.arange(buffer_rows, dtype=jnp.int32)
    hits = arrival_row[None, :] == buffer_range[:, None]
    back_index = jnp.sum(
        jnp.where(hits, jnp.arange(slots_piece, dtype=jnp.int32)[None, :], 0), axis=1
    )
    expert_out = jnp.take(summed, back_index, axis=1).reshape(
        column_width, expert_devices, seat_count
    )
    returned = lax.all_to_all(expert_out, "ep", split_axis=1, concat_axis=1, tiled=True)
    token_range = jnp.arange(local_tokens, dtype=jnp.int32)
    combine = jnp.where(
        (source_index[None, :] == token_range[:, None]) & filled[None, :], seat_weight[None, :], 0.0
    )
    mixed_out = jnp.einsum(
        "tb,cb->tc",
        combine,
        returned.reshape(column_width, buffer_rows).astype(jnp.float32),
        precision=lax.Precision.HIGHEST,
    )
    return mixed_out.astype(jnp.bfloat16)


def xor_pairs(size, mask):
    return [(a, a ^ mask) for a in range(size)]


def halving_order(bits):
    order = [0]
    for s in reversed(range(bits)):
        order = [p ^ (1 << s) for p in order] + order
    return order


def gate_up_kernel(parity, tok, row0, row1, n0, n1, wg, wu, recv, send, keep, own, far):
    half = send.shape[1]
    width = own.shape[1]

    @pl.when(pl.program_id(0) == 0)
    def _():
        pick0 = (tok[0] == row0[...]).astype(jnp.float32).astype(jnp.bfloat16)
        pick1 = (tok[0] == row1[...]).astype(jnp.float32).astype(jnp.bfloat16)
        rows = jnp.dot(pick0, n0[...], preferred_element_type=jnp.float32) + jnp.dot(
            pick1, n1[...], preferred_element_type=jnp.float32
        )
        even = parity[0] == 0
        low, high = rows[:, :width], rows[:, width:]
        own[...] = jnp.where(even, low, high).astype(jnp.bfloat16)
        far[...] = jnp.where(even, high, low).astype(jnp.bfloat16)

    for n, w in enumerate((wg, wu)):
        part = jnp.dot(own[...], w[0], preferred_element_type=jnp.float32) + jnp.dot(
            far[...], recv[n], preferred_element_type=jnp.float32
        )
        send[n] = part[:half].astype(jnp.bfloat16)
        keep[n] = part[half:]


def gate_up(q, start, parity, tok, row0, row1, n0, n1, wg, wu, recv):
    slots = tok.shape[1]
    width = wg.shape[1]
    units = recv.shape[2]
    step = units // 2
    rows = n0.shape[0]
    whole = lambda f, s: (0, 0)
    mine = pl.BlockSpec((1, width, step), lambda f, s: (2 * q + s[0], 0, start // step + f))
    half = slots // 2
    out = pl.BlockSpec((2, half, step), lambda f, s: (0, 0, f))
    return pl.pallas_call(
        gate_up_kernel,
        grid_spec=pltpu.PrefetchScalarGridSpec(
            num_scalar_prefetch=1,
            grid=(units // step,),
            in_specs=[
                pl.BlockSpec((1, slots, 1), lambda f, s: (q, 0, 0)),
                pl.BlockSpec((1, rows), whole),
                pl.BlockSpec((1, rows), whole),
                pl.BlockSpec(n0.shape, whole),
                pl.BlockSpec(n1.shape, whole),
                mine,
                mine,
                pl.BlockSpec((2, width, step), lambda f, s: (0, 0, f)),
            ],
            out_specs=[out, out],
            scratch_shapes=[pltpu.VMEM((slots, width), jnp.bfloat16)] * 2,
        ),
        out_shape=[
            jax.ShapeDtypeStruct((2, half, units), jnp.bfloat16),
            jax.ShapeDtypeStruct((2, half, units), jnp.float32),
        ],
    )(parity, tok, row0, row1, n0, n1, wg, wu, recv)


def down_kernel(parts, pieces, first, last, parity, *refs):
    count = parts * pieces
    tok, scale, order, wd, rd = refs[count : count + 5]
    rest = refs[count + 5 :]
    hidden = [
        jnp.concatenate([h[...] for h in refs[n * pieces : (n + 1) * pieces]], axis=0)
        for n in range(parts)
    ]
    units = wd.shape[2] // parts
    dims = (((1,), (1,)), ((), ()))
    pick = (order[...] == tok[0]).astype(jnp.float32).astype(jnp.bfloat16)
    width = wd.shape[1]
    for n, w in enumerate((wd, rd)):
        out = 0.0
        for m, h in enumerate(hidden):
            w_part = w[0, :, m * units : (m + 1) * units]
            out = out + lax.dot_general(h, w_part, dims, preferred_element_type=jnp.float32)
        out = (out * scale[0]).astype(jnp.bfloat16)
        part = jnp.dot(pick, out, preferred_element_type=jnp.float32)
        cols = slice(n * width, (n + 1) * width)
        if not first:
            part = part + rest[0][:, cols]
        if last:
            half = part.shape[0] // 2
            rest[-2][:, cols] = part[:half].astype(jnp.bfloat16)
            rest[-1][:, cols] = part[half:]
        else:
            rest[-1][:, cols] = part


def down(q, last, parity, hid, tok, scale, order, wd, rd, total):
    slots = tok.shape[2]
    width, units = wd.shape[1:]
    rows = order.shape[0]
    whole = lambda g, s: (0, 0)
    flat = [h for part in hid for h in part]
    in_specs = [pl.BlockSpec(h.shape, whole) for h in flat] + [
        pl.BlockSpec((1, 1, slots), lambda g, s: (q, 0, 0)),
        pl.BlockSpec((1, slots, 1), lambda g, s: (q, 0, 0)),
        pl.BlockSpec(order.shape, whole),
        pl.BlockSpec((1, width, units), lambda g, s: (2 * q + s[0], 0, 0)),
        pl.BlockSpec((1, width, units), lambda g, s: (0, 0, 0)),
    ]
    args = [parity, *flat, tok, scale, order, wd, rd]
    if total is not None:
        in_specs.append(pl.BlockSpec((rows, 2 * width), whole))
        args.append(total)
    if last:
        shape = (rows // 2, 2 * width)
        outs = [jax.ShapeDtypeStruct(shape, jnp.bfloat16), jax.ShapeDtypeStruct(shape, jnp.float32)]
    else:
        outs = [jax.ShapeDtypeStruct((rows, 2 * width), jnp.float32)]
    return pl.pallas_call(
        functools.partial(down_kernel, len(hid), len(hid[0]), total is None, last),
        grid_spec=pltpu.PrefetchScalarGridSpec(
            num_scalar_prefetch=1,
            grid=(1,),
            in_specs=in_specs,
            out_specs=[pl.BlockSpec(o.shape, whole) for o in outs],
        ),
        out_shape=outs,
    )(*args)


def sums_move(tokens, norm_gain, chosen, slot_weight, gate_weight, up_weight, down_weight):
    n_ep = lax.axis_size("ep")
    n_tp = lax.axis_size("tp")
    ep = lax.axis_index("ep")
    tp = lax.axis_index("tp")
    y, z = ep % 2, ep // 2
    core, x = tp % 2, tp // 2
    n_z = n_ep // 2
    bits = n_z.bit_length() - 1
    experts, slots = chosen.shape
    pairs = experts // 2
    tok_dev, _ = tokens.shape
    width = gate_weight.shape[1]
    half_rows = tok_dev // 2
    columns = 2 * width
    ep_swap = lambda v, mask: lax.ppermute(v, "ep", xor_pairs(n_ep, mask))
    core_swap = lambda v: lax.ppermute(v, "tp", xor_pairs(n_tp, 1))
    parity = y.astype(jnp.int32).reshape(1)

    def swap_y(ws, q, start, size):
        at = (2 * q + 1 - y, 0, start)
        piece = [lax.dynamic_slice(w, at, (1, width, size)) for w in ws]
        return ep_swap(jnp.concatenate(piece, axis=0), 1)

    values = lax.dynamic_slice_in_dim(tokens, core * half_rows, half_rows, 0).astype(jnp.float32)
    scaled = values * lax.rsqrt(jnp.mean(values * values, axis=1, keepdims=True) + EPSILON)
    normed = (scaled * norm_gain).astype(jnp.bfloat16)
    parts = []
    for p in range(n_z):
        part = lax.dynamic_slice_in_dim(normed, (z ^ p) * columns, columns, 1)
        parts.append(part if p == 0 else ep_swap(part, 2 * p))
    z_rows = jnp.concatenate(parts, axis=0)
    y_rows = ep_swap(z_rows, 1)
    n0 = jnp.concatenate([z_rows, y_rows], axis=0)
    n1 = core_swap(n0)
    r = jnp.arange(n0.shape[0], dtype=jnp.int32)
    owner = (z ^ (r // half_rows % n_z)) * 2 + (y ^ (r // (half_rows * n_z)))
    row0 = (owner * tok_dev + core * half_rows + r % half_rows)[None]
    row1 = (owner * tok_dev + (1 - core) * half_rows + r % half_rows)[None]

    order = halving_order(bits)

    def arrange(a):
        a = a.reshape(pairs, 2, n_z, slots // n_z)
        a = jnp.where(y == 0, a[:, 0], a[:, 1])
        for s in range(bits):
            b = a.reshape(pairs, n_z >> (s + 1), 2, 1 << s, slots // n_z)
            a = jnp.where((z >> s) % 2 == 0, b, jnp.flip(b, 2)).reshape(a.shape)
        return jnp.concatenate([a[:, p] for p in order], axis=1)

    tok = arrange(chosen)
    scale = arrange(slot_weight)
    tok_col, tok_row, scale_col = tok[:, :, None], tok[:, None, :], scale[:, :, None]

    yx = y * (n_tp // 2) + x
    n_far = n_ep // 2
    g = jnp.arange(n_ep * tok_dev, dtype=jnp.int32)
    side = jnp.where(g < n_far * tok_dev, 1 - core, core)
    sum_order = ((side * n_far + (yx ^ (g // tok_dev % n_far))) * tok_dev + g % tok_dev)[:, None]

    total = None
    hids = []
    units = gate_weight.shape[2]
    for q, n, parts in chunk_list(pairs):
        size = units // parts
        recv = swap_y((gate_weight, up_weight), q, n * size, size)
        send, keep = gate_up(
            q, n * size, parity, tok_col, row0, row1, n0, n1, gate_weight, up_weight, recv
        )
        for s in range(bits):
            got = ep_swap(send, 2 << s)
            keep = keep + got.astype(jnp.float32)
            if s + 1 < bits:
                half = keep.shape[1] // 2
                send, keep = keep[:, :half].astype(jnp.bfloat16), keep[:, half:]
        hidden = (jax.nn.silu(keep[0]) * keep[1]).astype(jnp.bfloat16)
        hids.append([hidden if p == 0 else ep_swap(hidden, 2 * p) for p in order])
        if n + 1 < parts:
            continue
        rd = swap_y((down_weight,), q, 0, units)
        last = q == pairs - 1
        outs = down(q, last, parity, hids, tok_row, scale_col, sum_order, down_weight, rd, total)
        total = outs[0]
        hids = []
    send, keep = outs
    both = keep + core_swap(send).astype(jnp.float32)
    both = both.astype(jnp.bfloat16).reshape(n_far, tok_dev, columns)
    mixed = 0.0
    for p in range(n_far):
        pairs_of = []
        for d in range(n_ep * n_tp):
            de, dt = d // n_tp, d % n_tp
            d_yx = de % 2 * (n_tp // 2) + dt // 2
            pairs_of.append((d, (dt % 2 * n_far + (d_yx ^ p)) * n_tp + de // 2))
        got = lax.ppermute(both[p], ("ep", "tp"), pairs_of).astype(jnp.float32)
        from_y = ((ep % n_far) ^ p) // (n_tp // 2)
        swapped = jnp.concatenate([got[:, width:], got[:, :width]], axis=1)
        mixed = mixed + jnp.where(from_y == 0, got, swapped)
    return mixed.astype(jnp.bfloat16)


def few_slots(n_ep, n_tp, experts, slots, width):
    power = n_ep >= 8 and n_ep & (n_ep - 1) == 0
    return (
        power
        and n_ep == 2 * n_tp
        and experts == n_ep
        and slots <= 2 * width
        and slots % (4 * n_ep) == 0
    )


def chunk_list(pairs):
    chunks = []
    for q in range(pairs):
        parts = 2 if q in (0, pairs - 1) else 1
        chunks += [(q, n, parts) for n in range(parts)]
    return chunks


def solution(mesh):
    in_specs = (
        P("ep", None),
        P(),
        P(),
        P(),
        P(None, "ep", "tp"),
        P(None, "ep", "tp"),
        P(None, "ep", "tp"),
    )
    out_specs = P("ep", "tp")
    n_ep, n_tp = mesh.shape["ep"], mesh.shape["tp"]
    mapped = functools.partial(
        jax.shard_map, mesh=mesh, in_specs=in_specs, out_specs=out_specs, check_vma=False
    )

    def step(*args):
        chosen, gate_weight = args[2], args[4]
        width = gate_weight.shape[1] // n_ep
        if not few_slots(n_ep, n_tp, *chosen.shape, width):
            return mapped(weights_move)(*args)
        return mapped(sums_move)(*args)

    return step
```
